32 devices in a mesh: rep: 2 (over x), fs: 4 (over z), tp: 4 (over y, core).
Axes of the slice: x: 2, y: 2, z: 4, core: 2. Of those that a mesh axis runs over, the one named last changes fastest.
Arguments:
- tokens: bfloat16 [4096, 2048], P(('rep', 'fs', 'tp')), may hold values from -6 to 6
- norm_gain: float32 [2048], replicated, may hold values from 0.1 to 1.9
- gate_weight: float32 [2048, 5632], P('fs', 'tp'), may hold values from -0.125 to 0.125
- gate_scale: float32 [5632], P('tp'), may hold values from 0.5 to 2
- up_weight: float32 [2048, 5632], P('fs', 'tp'), may hold values from -0.125 to 0.125
- up_scale: float32 [5632], P('tp'), may hold values from 0.5 to 2
- down_weight: float32 [5632, 2048], P('tp', 'fs'), may hold values from -0.078125 to 0.078125
- down_scale: float32 [2048], P('fs'), may hold values from 0.5 to 2
Outputs:
- mixed: bfloat16 [4096, 2048], P(('rep', 'fs', 'tp'))
The draws below stay inside these ranges and needn't reach their ends.
All inputs are finite; a program needn't handle non-finite values.
Results may differ from the reference program's by a relative error of at most 0.014.
Values may be sent and summed in bfloat16 or wider, within the bound.
No kernel may reach another device: no remote copies, remote signals or barrier semaphores. Data moves between devices by JAX's collectives and lax.ppermute only.
A program may use at most 64 MiB of HBM per device.

```python
import math
import jax
import jax.numpy as jnp
from jax import lax

D = 2048
FF = 5632
TOKENS = 4096
N_TP = 4


def block_levels(rng, dims, shards, low, top_value):
    def one(position, parts):
        steps = jax.random.uniform(jax.random.fold_in(jax.random.fold_in(rng, 6), position), (parts,), jnp.float32, low / len(shards), top_value / len(shards))
        return jnp.repeat(jnp.exp(steps), dims[position] // parts).reshape((-1,) + (1,) * (len(dims) - position - 1))

    factor_of = one(*shards[0])
    for cut in shards[1:]:
        factor_of = factor_of * one(*cut)
    return factor_of


def bell_draw(rng, shape, spread, limit, split=(), held_as=jnp.bfloat16):
    array = spread * jax.random.normal(rng, shape, jnp.float32)
    if split:
        array = array * block_levels(rng, shape, split, -0.22, 0.18)
    return jnp.clip(array, -limit, limit).astype(held_as)


def setup_inputs(seed: int = 0) -> dict:
    key_of = jax.random.split(jax.random.key(seed), 9)
    tokens = bell_draw(key_of[0], (TOKENS, D), 1.0, 6.0, ((0, 32),))
    norm_gain = jnp.clip(1.0 + 0.18 * jax.random.normal(key_of[1], (D,), jnp.float32), 0.1, 1.9)
    gate_weight = bell_draw(key_of[2], (D, FF), D ** -0.5, 0.125, ((0, 4), (1, 4)), jnp.float32)
    gate_scale = jnp.clip(jnp.exp(math.log(2.0) - 1.3862944 * jax.random.uniform(key_of[3], (FF,), jnp.float32) ** block_levels(key_of[3], (FF,), ((0, 4),), -0.2, 0.2)), 0.5, 2.0)
    up_weight = bell_draw(key_of[4], (D, FF), D ** -0.5, 0.125, ((0, 4), (1, 4)), jnp.float32)
    up_scale = jnp.clip(jnp.exp(math.log(2.0) - 1.3862944 * jax.random.uniform(key_of[5], (FF,), jnp.float32) ** block_levels(key_of[5], (FF,), ((0, 4),), -0.2, 0.2)), 0.5, 2.0)
    down_weight = bell_draw(key_of[6], (FF, D), FF ** -0.5, 0.078125, ((0, 4), (1, 4)), jnp.float32)
    down_scale = jnp.clip(jnp.exp(math.log(2.0) - 1.3862944 * jax.random.uniform(key_of[7], (D,), jnp.float32) ** block_levels(key_of[7], (D,), ((0, 4),), -0.2, 0.2)), 0.5, 2.0)
    return dict(tokens=tokens, norm_gain=norm_gain, gate_weight=gate_weight, gate_scale=gate_scale, up_weight=up_weight, up_scale=up_scale, down_weight=down_weight, down_scale=down_scale)


def reference(tokens, norm_gain, gate_weight, gate_scale, up_weight, up_scale, down_weight, down_scale):
    flat = tokens.astype(jnp.float32)
    mean_square = lax.optimization_barrier(jnp.mean(flat * flat, axis=-1, keepdims=True))
    inverse = jax.lax.rsqrt(mean_square + 1e-06)
    normed = (flat * inverse * norm_gain).astype(jnp.bfloat16)
    gate_low = gate_weight.astype(jnp.bfloat16)
    up_low = up_weight.astype(jnp.bfloat16)
    down_low = down_weight.astype(jnp.bfloat16)
    gate = jnp.dot(normed, gate_low, preferred_element_type=jnp.float32) * gate_scale
    up = jnp.dot(normed, up_low, preferred_element_type=jnp.float32) * up_scale
    hidden = (jax.nn.silu(gate) * up).astype(jnp.bfloat16)
    width = FF // N_TP
    total = jnp.zeros((tokens.shape[0], D), jnp.float32)
    for block in range(N_TP):
        part = jnp.dot(hidden[:, block * width:(block + 1) * width], down_low[block * width:(block + 1) * width, :], preferred_element_type=jnp.float32)
        total = total + part.astype(jnp.bfloat16).astype(jnp.float32)
    return (total * down_scale).astype(jnp.bfloat16)
```

```python
import functools

import jax
import jax.numpy as jnp
from jax import lax
from jax.experimental import pallas as pl
from jax.experimental.pallas import tpu as pltpu
from jax.sharding import PartitionSpec as P


AXES = ("rep", "fs", "tp")
VMEM_BYTES = 60 * 1024 * 1024
SCALE_ROWS = 16
ROWS_BY_ROWS = (((1,), (1,)), ((), ()))


def hidden_kernel(count, width, aligned, first, last, offsets, *refs):
    refs = list(refs)
    x = refs.pop(0)
    weights = [refs.pop(0) for _ in range(count)]
    sums = None if first else refs.pop(0)
    scales = refs.pop(0) if last else None
    out = refs.pop(0)
    totals = []
    for k in range(2):
        total = None if first else sums[k]
        for i in range(count):
            if aligned:
                part = x[:, pl.ds(pl.multiple_of(offsets[i], width), width)]
            else:
                part = x[:, i * width : (i + 1) * width]
            product = lax.dot_general(
                part, weights[i][k], ROWS_BY_ROWS, preferred_element_type=jnp.float32
            )
            total = product if total is None else total + product
        if not last:
            out[k] = total
        totals.append(total)
    if last:
        gate = totals[0] * scales[0:1, :]
        up = totals[1] * scales[1:2, :]
        out[...] = (gate / (1.0 + jnp.exp(-gate)) * up).astype(out.dtype)


def hidden_part(x, starts, pieces, sums, scales):
    rows, units, width = x.shape[0], pieces[0].shape[1], pieces[0].shape[2]
    first, last = sums is None, scales is not None
    aligned = width % 128 == 0
    if not aligned:
        x = jnp.concatenate([lax.dynamic_slice_in_dim(x, s, width, 1) for s in starts], axis=1)
    block = min(rows, 256)
    once = pl.Buffered(1)
    in_specs = [pl.BlockSpec((block, x.shape[1]), lambda i, o: (i, 0))]
    in_specs += [
        pl.BlockSpec(p.shape, lambda i, o: (0, 0, 0), pipeline_mode=once) for p in pieces
    ]
    operands = [x, *pieces]
    wide = pl.BlockSpec((2, block, units), lambda i, o: (0, i, 0))
    if not first:
        in_specs.append(wide)
        operands.append(sums)
    if last:
        in_specs.append(pl.BlockSpec((2, units), lambda i, o: (0, 0)))
        operands.append(scales)
        out_spec = pl.BlockSpec((block, units), lambda i, o: (i, 0))
        out_shape = jax.ShapeDtypeStruct((rows, units), jnp.bfloat16)
    else:
        out_spec = wide
        out_shape = jax.ShapeDtypeStruct((2, rows, units), jnp.float32)
    return pl.pallas_call(
        functools.partial(hidden_kernel, len(pieces), width, aligned, first, last),
        grid_spec=pltpu.PrefetchScalarGridSpec(
            num_scalar_prefetch=1,
            grid=(rows // block,),
            in_specs=in_specs,
            out_specs=out_spec,
        ),
        out_shape=out_shape,
        compiler_params=pltpu.CompilerParams(vmem_limit_bytes=VMEM_BYTES),
        cost_estimate=pl.CostEstimate(
            flops=4 * rows * width * len(pieces) * units,
            bytes_accessed=4 * width * len(pieces) * units + 8 * rows * units,
            transcendentals=0,
        ),
        name="hidden",
    )(jnp.stack(starts).astype(jnp.int32), *operands)


def plan_of(n):
    mirror, steps = n - 1, []
    for root in (0, mirror):
        held = [root]
        if root:
            steps.append((root, -1, mirror))
        bit = 1
        while bit < n // 2:
            for s in list(held):
                steps.append((s ^ bit, s, bit))
                held.append(s ^ bit)
            bit *= 2
    return steps


def shards(
    sizes,
    tokens,
    norm_gain,
    gate_weight,
    gate_scale,
    up_weight,
    up_scale,
    down_weight,
    down_scale,
):
    reps, n, n_tp = sizes
    half, n_y, mirror = n // 2, n_tp // 2, n - 1
    rep, f = lax.axis_index("rep"), lax.axis_index("fs")
    lower = f < half
    low = jnp.bfloat16
    plan = plan_of(n)
    slots = [0] + [step[0] for step in plan]

    def move(value, target):
        devices = [(r, z, k) for r in range(reps) for z in range(n) for k in range(n_tp)]
        pairs = [(i, devices.index(target(*d))) for i, d in enumerate(devices)]
        return lax.ppermute(value, AXES, pairs)

    def to_fs(offset):
        return lambda r, z, k: (r, z ^ offset, k)

    def to_rep(shift):
        return lambda r, z, k: ((r + shift) % reps, z, k)

    def to_core(r, z, k):
        return r, z, k ^ 1

    def to_y(shift):
        return lambda r, z, k: (r, z, ((k // 2 + shift) % n_y) * 2 + k % 2)

    def part_of(weight, mine, units_axis, q):
        count = weight.shape[units_axis] // 2
        first = lax.slice_in_dim(weight, 0, count, axis=units_axis)
        second = lax.slice_in_dim(weight, count, 2 * count, axis=units_axis)
        width = weight.shape[1 - units_axis] // reps
        start = ((rep - q) % reps) * width

        def cut(value):
            return lax.dynamic_slice_in_dim(value, start, width, 1 - units_axis)

        return jnp.where(lower == mine, cut(first), cut(second)).astype(low)

    def pair_part(mine, q):
        return jnp.stack([part_of(w, mine, 1, q).T for w in (gate_weight, up_weight)])

    top = down_scale.astype(low)
    rest = down_scale - top.astype(jnp.float32)
    middle = rest.astype(low)
    bottom = (rest - middle.astype(jnp.float32)).astype(low)
    terms = jnp.concatenate(
        [jnp.stack([top, middle, bottom]), jnp.zeros((SCALE_ROWS - 3, top.shape[0]), low)]
    )

    def down_piece(mine, q):
        width = terms.shape[1] // reps
        own = lax.dynamic_slice_in_dim(terms, ((rep - q) % reps) * width, width, 1)
        return jnp.concatenate([part_of(down_weight, mine, 0, q), own])

    def line(part):
        carried = {0: part(True, 0), -1: part(False, 0)}
        for s, source, offset in plan:
            carried[s] = move(carried[source], to_fs(offset))
        blocks = {0: [carried[0]] + [part(True, q) for q in range(1, reps)]}
        for s in slots[1:]:
            blocks[s] = [carried[s]] + [move(carried[s], to_rep(q)) for q in range(1, reps)]
        return blocks

    flat = tokens.astype(jnp.float32)
    mean_square = jnp.mean(flat * flat, axis=-1, keepdims=True)
    inverse = lax.rsqrt(mean_square + 1e-06)
    normed = (flat * inverse * norm_gain).astype(low)
    rows, depth = normed.shape
    own, other = [], []
    for base in (normed, move(normed, to_fs(mirror))):
        across_y = [base] + [move(base, to_y(-k)) for k in range(1, n_y)]
        across_y = jnp.concatenate(across_y)
        own.append(across_y)
        other.append(move(across_y, to_core))
    group = jnp.concatenate(own + other)

    pairs = line(pair_part)
    downs = line(down_piece)

    k_block = gate_weight.shape[0]
    k_piece = k_block // reps

    def some(chosen):
        starts = [
            (f ^ s) * k_block + ((rep - q) % reps) * k_piece for s in chosen for q in range(reps)
        ]
        return starts, [p for s in chosen for p in pairs[s]]

    scale_pair = jnp.stack([gate_scale, up_scale])
    units = scale_pair.shape[1] // 2
    scale_pair = jnp.where(lower, scale_pair[:, :units], scale_pair[:, units:])
    sums = hidden_part(group, *some(slots[:-1]), None, None)
    hidden = hidden_part(group, *some(slots[-1:]), sums, scale_pair)
    hidden_own, hidden_other = jnp.split(hidden, 2)

    def product(value, s):
        return jnp.concatenate(
            [
                jnp.dot(value, d[:units], preferred_element_type=jnp.float32).astype(low)
                for d in downs[s]
            ],
            axis=1,
        )

    kept, back = {}, {}
    for s in slots:
        total = move(product(hidden_other, s), to_core).astype(jnp.float32)
        total += product(hidden_own, s).astype(jnp.float32)
        total = total.reshape(2, n_y, rows, total.shape[-1])
        sent = total[:, 1:].astype(low)
        total = total[:, 0]
        for k in range(1, n_y):
            total += move(sent[:, k - 1], to_y(k)).astype(jnp.float32)
        kept[s] = total[0]
        back[s] = move(total[1].astype(low), to_fs(mirror))

    n_block = down_weight.shape[1]
    n_piece = n_block // reps
    mixed = jnp.zeros((rows, depth), low)
    for s in slots:
        total = kept[s] + back[s ^ mirror].astype(jnp.float32)
        for q in range(reps):
            scale = jnp.sum(downs[s][q][units : units + 3].astype(jnp.float32), axis=0)
            piece = (total[:, q * n_piece : (q + 1) * n_piece] * scale).astype(low)
            start = (f ^ s) * n_block + ((rep - q) % reps) * n_piece
            mixed = lax.dynamic_update_slice(mixed, piece, (0, start))
    return mixed


def layer(sizes, *args):
    return shards(sizes, *args)


def solution(mesh):
    in_specs = (
        P(("rep", "fs", "tp"), None),
        P(),
        P("fs", "tp"),
        P("tp"),
        P("fs", "tp"),
        P("tp"),
        P("tp", "fs"),
        P("fs"),
    )
    out_specs = P(("rep", "fs", "tp"), None)
    sizes = tuple(mesh.shape[name] for name in AXES)
    body = functools.partial(layer, sizes)
    return jax.shard_map(body, mesh=mesh, in_specs=in_specs, out_specs=out_specs, check_vma=False)
```
